32 devices in a mesh: fs: 8 (over z, x), tp: 4 (over y, core).
Axes of the slice: x: 2, y: 2, z: 4, core: 2. Of those that a mesh axis runs over, the one named last changes fastest.
Arguments:
- tokens: bfloat16 [8192, 2048], P('fs'), may hold values from -3 to 3
- gate_weight: bfloat16 [2048, 5632], P('fs', 'tp'), may hold values from -0.125 to 0.125
- value_weight: bfloat16 [2048, 5632], P('fs', 'tp'), may hold values from -0.125 to 0.125
- gate_taps: bfloat16 [3, 5632], P(None, 'tp'), may hold values from -3 to 3
- value_taps: bfloat16 [3, 5632], P(None, 'tp'), may hold values from -3 to 3
- down_weight: bfloat16 [5632, 2048], P('tp', 'fs'), may hold values from -0.078125 to 0.078125
- norm_gain: float32 [2048], replicated, may hold values from 0.1 to 1.9
- norm_bias: float32 [2048], replicated, may hold values from -3 to 3
Outputs:
- normed: bfloat16 [8192, 2048], P('fs')
The draws below stay inside these ranges and needn't reach their ends.
All inputs are finite; a program needn't handle non-finite values.
Results may differ from the reference program's by a relative error of at most 0.005.
Values may be sent and summed in bfloat16 or wider, within the bound.
A program may use at most 64 MiB of HBM per device.

```python
import jax
import jax.numpy as jnp
from jax import lax

D = 2048
FF = 5632
TOK_DEV = 1024
TOKENS = 8192
N_FS = 8
N_TP = 4


def block_scale(rng, dims, shards, least, high):
    def one(position, blocks):
        heights = jax.random.uniform(jax.random.fold_in(jax.random.fold_in(rng, 6), position), (blocks,), jnp.float32, least / len(shards), high / len(shards))
        return jnp.repeat(jnp.exp(heights), dims[position] // blocks).reshape((-1,) + (1,) * (len(dims) - position - 1))

    factor_of = one(*shards[0])
    for cut in shards[1:]:
        factor_of = factor_of * one(*cut)
    return factor_of


def scatter_about(key, dims, deviation, limit, pieces=(), held_as=jnp.bfloat16):
    result = jax.random.normal(key, dims, jnp.float32) * deviation
    if len(pieces) > 0:
        result = block_scale(key, dims, pieces, -0.22, 0.18) * result
    return jnp.clip(result, min=-limit, max=limit).astype(held_as)


def setup_inputs(seed: int = 0) -> dict:
    streams_of = jax.random.split(jax.random.key(seed), 9)
    return {
        "tokens": scatter_about(streams_of[0], (TOKENS, D), 0.5, 3.0, ((0, 8),)),
        "gate_weight": scatter_about(streams_of[1], (D, FF), D ** -0.5, 0.125, ((0, 8), (1, 4))),
        "value_weight": scatter_about(streams_of[2], (D, FF), D ** -0.5, 0.125, ((0, 8), (1, 4))),
        "gate_taps": scatter_about(streams_of[3], (3, FF), 0.577, 3.0, ((1, 4),)),
        "value_taps": scatter_about(streams_of[4], (3, FF), 0.577, 3.0, ((1, 4),)),
        "down_weight": scatter_about(streams_of[5], (FF, D), FF ** -0.5, 0.078125, ((0, 4), (1, 8))),
        "norm_gain": jnp.clip(1.0 + 0.18 * jax.random.normal(streams_of[6], (D,), jnp.float32), 0.1, 1.9),
        "norm_bias": scatter_about(streams_of[7], (D,), 0.5, 3.0, (), jnp.float32),
    }


EPSILON = 1e-05
RESIDUAL_SCALE = 8.0 ** 0.25

def rounded(values):
    return lax.optimization_barrier(values.astype(jnp.bfloat16)).astype(jnp.float32)

def centred_conv(values, taps):
    padded = jnp.pad(values, ((0, 0), (1, 1), (0, 0)))
    return padded[:, :-2] * taps[0] + padded[:, 1:-1] * taps[1] + padded[:, 2:] * taps[2]

def reference(tokens, gate_weight, value_weight, gate_taps, value_taps, down_weight, norm_gain, norm_bias):
    gate_lin = rounded(jnp.dot(tokens, gate_weight, preferred_element_type=jnp.float32))
    value_lin = rounded(jnp.dot(tokens, value_weight, preferred_element_type=jnp.float32))
    layout = (N_FS, TOK_DEV, FF)
    gate_conv = centred_conv(gate_lin.reshape(layout), gate_taps.astype(jnp.float32))
    value_conv = centred_conv(value_lin.reshape(layout), value_taps.astype(jnp.float32))
    hidden = (jax.nn.silu(gate_conv) * value_conv).astype(jnp.bfloat16).reshape(TOKENS, FF)
    block_width = FF // N_TP

    def add_block(summed, index):
        columns = lax.dynamic_slice_in_dim(hidden, index * block_width, block_width, 1)
        weight_rows = lax.dynamic_slice_in_dim(down_weight, index * block_width, block_width, 0)
        partial_value = jnp.dot(columns, weight_rows, preferred_element_type=jnp.float32)
        return (summed + rounded(partial_value), None)
    summed, _ = lax.scan(add_block, jnp.zeros((TOKENS, D), jnp.float32), jnp.arange(N_TP, dtype=jnp.int32))
    mixed = RESIDUAL_SCALE * tokens.astype(jnp.float32) + rounded(summed)
    centered = mixed - lax.optimization_barrier(jnp.mean(mixed, -1, keepdims=True))
    variance = lax.optimization_barrier(jnp.mean(centered * centered, -1, keepdims=True))
    normed = centered * lax.rsqrt(variance + EPSILON) * norm_gain + norm_bias
    return normed.astype(jnp.bfloat16)
```

```python
import functools

import jax
import jax.numpy as jnp
from jax import lax
from jax.experimental import pallas as pl
from jax.experimental.pallas import tpu as pltpu
from jax.sharding import PartitionSpec as P

EPSILON = 1e-05
RESIDUAL_SCALE = 8.0**0.25
LANES = 128
VMEM_BYTES = 67043328


def rounded(values):
    return lax.optimization_barrier(values.astype(jnp.bfloat16)).astype(jnp.float32)


def centred_conv(values, taps):
    padded = jnp.pad(values, ((1, 1), (0, 0)))
    return padded[:-2] * taps[0] + padded[1:-1] * taps[1] + padded[2:] * taps[2]


def finish(summed, residual, norm_gain, norm_bias):
    mixed = RESIDUAL_SCALE * residual.astype(jnp.float32) + rounded(summed)
    centered = mixed - jnp.mean(mixed, -1, keepdims=True)
    variance = jnp.mean(centered * centered, -1, keepdims=True)
    normed = centered * lax.rsqrt(variance + EPSILON) * norm_gain + norm_bias
    return normed.astype(jnp.bfloat16)


def collective_form(
    tokens, gate_weight, value_weight, gate_taps, value_taps, down_weight, norm_gain, norm_bias
):
    def add_rows(portion):
        return jnp.dot(tokens, portion, preferred_element_type=jnp.float32)

    gate_sum = add_rows(lax.all_gather(gate_weight, "fs", axis=0, tiled=True))
    value_sum = add_rows(lax.all_gather(value_weight, "fs", axis=0, tiled=True))
    gate_conv = centred_conv(rounded(gate_sum), gate_taps.astype(jnp.float32))
    value_conv = centred_conv(rounded(value_sum), value_taps.astype(jnp.float32))
    hidden = (jax.nn.silu(gate_conv) * value_conv).astype(jnp.bfloat16)
    partials = rounded(
        jnp.dot(
            hidden,
            lax.all_gather(down_weight, "fs", axis=1, tiled=True),
            preferred_element_type=jnp.float32,
        )
    )
    shares = lax.psum_scatter(
        partials.astype(jnp.bfloat16), "tp", scatter_dimension=0, tiled=True
    ).astype(jnp.float32)
    share_rows = shares.shape[0]
    own_rows = lax.dynamic_slice_in_dim(tokens, lax.axis_index("tp") * share_rows, share_rows, 0)
    normed_share = finish(shares, own_rows, norm_gain, norm_bias)
    return lax.all_gather(normed_share, "tp", axis=0, tiled=True)


def branch_kernel(
    n, t_ref, g_ref, v_ref, gt_ref, vt_ref, d_ref, out_ref,
    gbuf, vbuf, dbuf, acc_g, acc_v, hid, pbuf, rbuf, cbuf, ybuf, obuf,
    w_send, w_recv, c_send, c_recv, y_send, y_recv, o_send, o_recv,
):
    rows, units = hid.shape
    half_rows = rows // 2
    tile = 256
    fs = lax.axis_index("fs")
    tp = lax.axis_index("tp")
    core = lax.rem(tp, 2)
    partner = tp + 1 - 2 * core
    across = lax.rem(tp + 2, 4)
    half_n = n // 2

    x, z = lax.rem(fs, 2), lax.div(fs, 2)
    pos = (1 - x) * z + x * (n - 1 - z)

    def at_pos(p):
        p = lax.rem(p, n)
        down = lax.div(p, half_n)
        return (1 - down) * 2 * p + down * (2 * (n - 1 - p) + 1)

    right, left = at_pos(pos + 1), at_pos(pos + n - 1)

    barrier = pltpu.get_barrier_semaphore()
    for target in ({"fs": left}, {"fs": right}, {"tp": partner}, {"tp": across}):
        pl.semaphore_signal(
            barrier, inc=1, device_id=target, device_id_type=pl.DeviceIdType.MESH
        )
    pl.semaphore_wait(barrier, 4)

    streams = ((g_ref, gbuf), (v_ref, vbuf), (d_ref, dbuf))

    def hop(stream, way, step, first=False):
        own, slots = streams[stream]
        part = pl.ds(way * LANES, LANES)
        where = (slice(None), part) if stream == 2 else (part, slice(None))
        source = own.at[where] if first else slots.at[(step - 1,) + where]
        k = stream * 2 + way
        return pltpu.make_async_remote_copy(
            src_ref=source,
            dst_ref=slots.at[(step,) + where],
            send_sem=w_send.at[k, step],
            recv_sem=w_recv.at[k, step],
            device_id={"fs": right if way == 0 else left},
            device_id_type=pl.DeviceIdType.MESH,
        )

    def begin(stream):
        for way in range(2):
            hop(stream, way, 0, True).start()

    def arrive(stream, step):
        for way in range(2):
            hop(stream, way, step - 1, True).wait_recv()

            @pl.when(step < n - 1)
            def _():
                hop(stream, way, step).start()

    begin(0)
    begin(1)

    def token_tile(r, step):
        row = pl.ds(pl.multiple_of(r * tile, tile), tile)
        a = pl.multiple_of(at_pos(pos + n - step) * 2 * LANES, LANES)
        b = pl.multiple_of(at_pos(pos + step) * 2 * LANES + LANES, LANES)
        return row, jnp.concatenate(
            [t_ref[row, pl.ds(a, LANES)], t_ref[row, pl.ds(b, LANES)]], axis=1
        )

    @pl.loop(0, rows // tile)
    def _(r):
        row, lhs = token_tile(r, 0)
        acc_g[row, :] = jnp.dot(lhs, g_ref[...], preferred_element_type=jnp.float32)
        acc_v[row, :] = jnp.dot(lhs, v_ref[...], preferred_element_type=jnp.float32)

    @pl.loop(1, n)
    def _(step):
        @pl.when(step == n - 1)
        def _():
            arrive(2, 1)

        arrive(0, step)
        arrive(1, step)

        @pl.when(step == n - 3)
        def _():
            begin(2)

        @pl.loop(0, rows // tile)
        def _(r):
            row, lhs = token_tile(r, step)
            acc_g[row, :] += jnp.dot(lhs, gbuf[step - 1], preferred_element_type=jnp.float32)
            acc_v[row, :] += jnp.dot(lhs, vbuf[step - 1], preferred_element_type=jnp.float32)

    row_id = lax.broadcasted_iota(jnp.int32, (rows, LANES), 0)

    def conv(acc, taps, cols):
        v = acc[:, cols].astype(jnp.bfloat16).astype(jnp.float32)
        c = taps[:, cols].astype(jnp.float32)
        before = jnp.where(row_id == 0, 0.0, pltpu.roll(v, 1, 0))
        after = jnp.where(row_id == rows - 1, 0.0, pltpu.roll(v, rows - 1, 0))
        return before * c[0:1] + v * c[1:2] + after * c[2:3]

    chunks = units // LANES

    @pl.loop(0, chunks)
    def _(i):
        cols = pl.ds(pl.multiple_of(i * LANES, LANES), LANES)
        gate = conv(acc_g, gt_ref, cols)
        value = conv(acc_v, vt_ref, cols)
        hid[:, cols] = (gate / (1.0 + jnp.exp(-gate)) * value).astype(jnp.bfloat16)

        @pl.when(i == chunks // 2)
        def _():
            arrive(2, 2)

    mine = pl.ds(pl.multiple_of(core * half_rows, half_rows), half_rows)
    other = pl.ds(pl.multiple_of((1 - core) * half_rows, half_rows), half_rows)

    def to_partner(step):
        return pltpu.make_async_remote_copy(
            src_ref=pbuf.at[step, other],
            dst_ref=rbuf.at[step],
            send_sem=c_send.at[step],
            recv_sem=c_recv.at[step],
            device_id={"tp": partner},
            device_id_type=pl.DeviceIdType.MESH,
        )

    def to_across(step):
        return pltpu.make_async_remote_copy(
            src_ref=cbuf.at[step],
            dst_ref=ybuf.at[step],
            send_sem=y_send.at[step],
            recv_sem=y_recv.at[step],
            device_id={"tp": across},
            device_id_type=pl.DeviceIdType.MESH,
        )

    def out_cols(step, way):
        owner = at_pos(pos + n - step) if way == 0 else at_pos(pos + step)
        return pl.ds(pl.multiple_of(owner * 2 * LANES + way * LANES, LANES), LANES)

    def to_out(step, way, where):
        cols = out_cols(step, way)
        return pltpu.make_async_remote_copy(
            src_ref=obuf.at[step, :, pl.ds(way * LANES, LANES)],
            dst_ref=out_ref.at[where, cols],
            send_sem=o_send.at[way, step],
            recv_sem=o_recv.at[way, step],
            device_id={"tp": partner},
            device_id_type=pl.DeviceIdType.MESH,
        )

    def project(step, weight):
        @pl.loop(0, rows // tile)
        def _(r):
            row = pl.ds(pl.multiple_of(r * tile, tile), tile)
            pbuf[step, row, :] = jnp.dot(
                hid[row, :], weight, preferred_element_type=jnp.float32
            ).astype(jnp.bfloat16)

        to_partner(step).start()
        to_partner(step).wait_recv()
        cbuf[step] = (
            pbuf[step, mine].astype(jnp.float32) + rbuf[step].astype(jnp.float32)
        ).astype(jnp.bfloat16)
        to_across(step).start()

    def settle(step):
        to_across(step).wait_recv()
        total = (
            cbuf[step].astype(jnp.float32) + ybuf[step].astype(jnp.float32)
        ).astype(jnp.bfloat16)
        obuf[step] = total
        for way in range(2):
            to_out(step, way, mine).start()
            out_ref[mine, out_cols(step, way)] = total[:, way * LANES:(way + 1) * LANES]

    project(0, d_ref[...])

    @pl.loop(1, n)
    def _(step):
        @pl.when(step > 2)
        def _():
            arrive(2, step)

        project(step, dbuf[step - 1])

        @pl.when(step >= 2)
        def _():
            settle(step - 2)

    settle(n - 2)
    settle(n - 1)

    @pl.loop(0, n - 1)
    def _(step):
        for stream in range(3):
            for way in range(2):
                hop(stream, way, step, True).wait_send()

    @pl.loop(0, n)
    def _(step):
        to_partner(step).wait_send()
        to_across(step).wait_send()
        for way in range(2):
            to_out(step, way, mine).wait_send()
            to_out(step, way, other).wait_recv()


def norm_kernel(b_ref, t_ref, gain_ref, bias_ref, out_ref):
    mixed = RESIDUAL_SCALE * t_ref[...].astype(jnp.float32) + b_ref[...].astype(jnp.float32)
    centered = mixed - jnp.mean(mixed, -1, keepdims=True)
    variance = jnp.mean(centered * centered, -1, keepdims=True)
    normed = centered * lax.rsqrt(variance + EPSILON) * gain_ref[...] + bias_ref[...]
    out_ref[...] = normed.astype(jnp.bfloat16)


def kernel_form(
    n, tokens, gate_weight, value_weight, gate_taps, value_taps, down_weight, norm_gain, norm_bias
):
    rows, width = tokens.shape
    depth, units = gate_weight.shape
    bf16, f32 = jnp.bfloat16, jnp.float32
    dma = pltpu.SemaphoreType.DMA
    branch = pl.pallas_call(
        functools.partial(branch_kernel, n),
        out_shape=jax.ShapeDtypeStruct((rows, width), bf16),
        in_specs=[pl.BlockSpec(memory_space=pltpu.VMEM)] * 6,
        out_specs=pl.BlockSpec(memory_space=pltpu.VMEM),
        scratch_shapes=[
            pltpu.VMEM((n - 1, depth, units), bf16),
            pltpu.VMEM((n - 1, depth, units), bf16),
            pltpu.VMEM((n - 1, units, depth), bf16),
            pltpu.VMEM((rows, units), f32),
            pltpu.VMEM((rows, units), f32),
            pltpu.VMEM((rows, units), bf16),
            pltpu.VMEM((n, rows, depth), bf16),
            pltpu.VMEM((n, rows // 2, depth), bf16),
            pltpu.VMEM((n, rows // 2, depth), bf16),
            pltpu.VMEM((n, rows // 2, depth), bf16),
            pltpu.VMEM((n, rows // 2, depth), bf16),
            dma((6, n - 1)),
            dma((6, n - 1)),
            dma((n,)),
            dma((n,)),
            dma((n,)),
            dma((n,)),
            dma((2, n)),
            dma((2, n)),
        ],
        compiler_params=pltpu.CompilerParams(
            collective_id=0, has_side_effects=True, vmem_limit_bytes=VMEM_BYTES
        ),
        name="branch",
    )(tokens, gate_weight, value_weight, gate_taps, value_taps, down_weight)
    block = 256
    by_rows = pl.BlockSpec((block, width), lambda i: (i, 0))
    whole = pl.BlockSpec((1, width), lambda i: (0, 0))
    return pl.pallas_call(
        norm_kernel,
        grid=(rows // block,),
        out_shape=jax.ShapeDtypeStruct((rows, width), bf16),
        in_specs=[by_rows, by_rows, whole, whole],
        out_specs=by_rows,
        name="norm",
    )(branch, tokens, norm_gain.reshape(1, width), norm_bias.reshape(1, width))


def solution(mesh):
    n_fs, n_tp = mesh.shape["fs"], mesh.shape["tp"]

    def on_device(tokens, gate_weight, *rest):
        rows = tokens.shape[0]
        depth, units = gate_weight.shape
        fits = n_tp == 4 and n_fs % 2 == 0 and n_fs >= 6
        fits = fits and depth == 2 * LANES and units % LANES == 0 and rows % 512 == 0
        if fits:
            return kernel_form(n_fs, tokens, gate_weight, *rest)
        return collective_form(tokens, gate_weight, *rest)

    return jax.shard_map(
        on_device,
        mesh=mesh,
        in_specs=(
            P("fs", None),
            P("fs", "tp"),
            P("fs", "tp"),
            P(None, "tp"),
            P(None, "tp"),
            P("tp", "fs"),
            P(None),
            P(None),
        ),
        out_specs=P("fs", None),
        check_vma=False,
    )
```

```python
import functools

import jax
import jax.numpy as jnp
from jax import lax
from jax.experimental import pallas as pl
from jax.experimental.pallas import tpu as pltpu
from jax.sharding import PartitionSpec as P

EPSILON = 1e-05
RESIDUAL_SCALE = 8.0**0.25
LANES = 128
VMEM_BYTES = 67043328


def rounded(values):
    return lax.optimization_barrier(values.astype(jnp.bfloat16)).astype(jnp.float32)


def centred_conv(values, taps):
    padded = jnp.pad(values, ((1, 1), (0, 0)))
    return padded[:-2] * taps[0] + padded[1:-1] * taps[1] + padded[2:] * taps[2]


def finish(summed, residual, norm_gain, norm_bias):
    mixed = RESIDUAL_SCALE * residual.astype(jnp.float32) + rounded(summed)
    centered = mixed - jnp.mean(mixed, -1, keepdims=True)
    variance = jnp.mean(centered * centered, -1, keepdims=True)
    normed = centered * lax.rsqrt(variance + EPSILON) * norm_gain + norm_bias
    return normed.astype(jnp.bfloat16)


def collective_form(
    tokens, gate_weight, value_weight, gate_taps, value_taps, down_weight, norm_gain, norm_bias
):
    def add_rows(portion):
        return jnp.dot(tokens, portion, preferred_element_type=jnp.float32)

    gate_sum = add_rows(lax.all_gather(gate_weight, "fs", axis=0, tiled=True))
    value_sum = add_rows(lax.all_gather(value_weight, "fs", axis=0, tiled=True))
    gate_conv = centred_conv(rounded(gate_sum), gate_taps.astype(jnp.float32))
    value_conv = centred_conv(rounded(value_sum), value_taps.astype(jnp.float32))
    hidden = (jax.nn.silu(gate_conv) * value_conv).astype(jnp.bfloat16)
    partials = rounded(
        jnp.dot(
            hidden,
            lax.all_gather(down_weight, "fs", axis=1, tiled=True),
            preferred_element_type=jnp.float32,
        )
    )
    shares = lax.psum_scatter(
        partials.astype(jnp.bfloat16), "tp", scatter_dimension=0, tiled=True
    ).astype(jnp.float32)
    share_rows = shares.shape[0]
    own_rows = lax.dynamic_slice_in_dim(tokens, lax.axis_index("tp") * share_rows, share_rows, 0)
    normed_share = finish(shares, own_rows, norm_gain, norm_bias)
    return lax.all_gather(normed_share, "tp", axis=0, tiled=True)


def branch_kernel(
    n, t_hbm, g_ref, v_ref, gt_ref, vt_ref, d_ref, out_ref,
    t_ref, gbuf, vbuf, dbuf, acc_g, acc_v, hid, pbuf, rbuf, cbuf, ybuf, obuf,
    w_send, w_recv, c_send, c_recv, y_send, y_recv, o_send, o_recv, t_sem,
):
    rows, units = hid.shape
    half_rows = rows // 2
    tile = 256
    fs = lax.axis_index("fs")
    tp = lax.axis_index("tp")
    core = lax.rem(tp, 2)
    partner = tp + 1 - 2 * core
    across = lax.rem(tp + 2, 4)
    half_n = n // 2

    x, z = lax.rem(fs, 2), lax.div(fs, 2)
    pos = (1 - x) * z + x * (n - 1 - z)

    def at_pos(p):
        p = lax.rem(p, n)
        down = lax.div(p, half_n)
        return (1 - down) * 2 * p + down * (2 * (n - 1 - p) + 1)

    right, left = at_pos(pos + 1), at_pos(pos + n - 1)

    barrier = pltpu.get_barrier_semaphore()
    for target in ({"fs": left}, {"fs": right}, {"tp": partner}, {"tp": across}):
        pl.semaphore_signal(
            barrier, inc=1, device_id=target, device_id_type=pl.DeviceIdType.MESH
        )
    pl.semaphore_wait(barrier, 4)

    streams = ((g_ref, gbuf), (v_ref, vbuf), (d_ref, dbuf), (d_ref, dbuf))
    half_units = units // 2

    def hop(stream, way, step, first=False):
        own, slots = streams[stream]
        part = pl.ds(way * LANES, LANES)
        where = (part, slice(None))
        if stream >= 2:
            where = (pl.ds((stream - 2) * half_units, half_units), part)
        source = own.at[where] if first else slots.at[(step - 1,) + where]
        k = stream * 2 + way
        return pltpu.make_async_remote_copy(
            src_ref=source,
            dst_ref=slots.at[(step,) + where],
            send_sem=w_send.at[k, step],
            recv_sem=w_recv.at[k, step],
            device_id={"fs": right if way == 0 else left},
            device_id_type=pl.DeviceIdType.MESH,
        )

    def begin(stream):
        for way in range(2):
            hop(stream, way, 0, True).start()

    def arrive(stream, step):
        for way in range(2):
            hop(stream, way, step - 1, True).wait_recv()

            @pl.when(step < n - 1)
            def _():
                hop(stream, way, step).start()

    begin(0)
    begin(1)
    load = pltpu.make_async_copy(t_hbm, t_ref, t_sem)
    load.start()
    load.wait()

    def token_tile(r, step):
        row = pl.ds(pl.multiple_of(r * tile, tile), tile)
        a = pl.multiple_of(at_pos(pos + n - step) * 2 * LANES, LANES)
        b = pl.multiple_of(at_pos(pos + step) * 2 * LANES + LANES, LANES)
        return row, jnp.concatenate(
            [t_ref[row, pl.ds(a, LANES)], t_ref[row, pl.ds(b, LANES)]], axis=1
        )

    @pl.loop(0, rows // tile)
    def _(r):
        row, lhs = token_tile(r, 0)
        acc_g[row, :] = jnp.dot(lhs, g_ref[...], preferred_element_type=jnp.float32)
        acc_v[row, :] = jnp.dot(lhs, v_ref[...], preferred_element_type=jnp.float32)

    @pl.loop(1, n)
    def _(step):
        arrive(0, step)
        arrive(1, step)

        @pl.when(step == n - 2)
        def _():
            begin(2)
            begin(3)

        @pl.loop(0, rows // tile)
        def _(r):
            row, lhs = token_tile(r, step)
            acc_g[row, :] += jnp.dot(lhs, gbuf[step - 1], preferred_element_type=jnp.float32)
            acc_v[row, :] += jnp.dot(lhs, vbuf[step - 1], preferred_element_type=jnp.float32)

    row_id = lax.broadcasted_iota(jnp.int32, (rows, LANES), 0)

    def conv(acc, taps, cols):
        v = acc[:, cols].astype(jnp.bfloat16).astype(jnp.float32)
        c = taps[:, cols].astype(jnp.float32)
        before = jnp.where(row_id == 0, 0.0, pltpu.roll(v, 1, 0))
        after = jnp.where(row_id == rows - 1, 0.0, pltpu.roll(v, rows - 1, 0))
        return before * c[0:1] + v * c[1:2] + after * c[2:3]

    chunks = units // LANES

    @pl.loop(0, chunks)
    def _(i):
        cols = pl.ds(pl.multiple_of(i * LANES, LANES), LANES)
        gate = conv(acc_g, gt_ref, cols)
        value = conv(acc_v, vt_ref, cols)
        hid[:, cols] = (gate / (1.0 + jnp.exp(-gate)) * value).astype(jnp.bfloat16)

        @pl.when(i == chunks // 4)
        def _():
            arrive(2, 1)

        @pl.when(i == chunks // 2)
        def _():
            arrive(3, 1)

        @pl.when(i == chunks - 2)
        def _():
            arrive(2, 2)

    mine = pl.ds(pl.multiple_of(core * half_rows, half_rows), half_rows)
    other = pl.ds(pl.multiple_of((1 - core) * half_rows, half_rows), half_rows)

    def to_partner(step):
        return pltpu.make_async_remote_copy(
            src_ref=pbuf.at[step, other],
            dst_ref=rbuf.at[step],
            send_sem=c_send.at[step],
            recv_sem=c_recv.at[step],
            device_id={"tp": partner},
            device_id_type=pl.DeviceIdType.MESH,
        )

    def to_across(step):
        return pltpu.make_async_remote_copy(
            src_ref=cbuf.at[step],
            dst_ref=ybuf.at[step],
            send_sem=y_send.at[step],
            recv_sem=y_recv.at[step],
            device_id={"tp": across},
            device_id_type=pl.DeviceIdType.MESH,
        )

    def out_cols(step, way):
        owner = at_pos(pos + n - step) if way == 0 else at_pos(pos + step)
        return pl.ds(pl.multiple_of(owner * 2 * LANES + way * LANES, LANES), LANES)

    def to_out(step, way, where):
        cols = out_cols(step, way)
        return pltpu.make_async_remote_copy(
            src_ref=obuf.at[step, :, pl.ds(way * LANES, LANES)],
            dst_ref=out_ref.at[where, cols],
            send_sem=o_send.at[way, step],
            recv_sem=o_recv.at[way, step],
            device_id={"tp": partner},
            device_id_type=pl.DeviceIdType.MESH,
        )

    def project(step, weight):
        def rows_from(first):
            @pl.loop(0, half_rows // tile)
            def _(r):
                row = pl.ds(pl.multiple_of(first * half_rows + r * tile, tile), tile)
                pbuf[step, row, :] = jnp.dot(
                    hid[row, :], weight, preferred_element_type=jnp.float32
                ).astype(jnp.bfloat16)

        rows_from(1 - core)
        to_partner(step).start()
        rows_from(core)

    def pair(step):
        to_partner(step).wait_recv()
        cbuf[step] = (
            pbuf[step, mine].astype(jnp.float32) + rbuf[step].astype(jnp.float32)
        ).astype(jnp.bfloat16)
        to_across(step).start()

    def settle(step):
        to_across(step).wait_recv()
        total = (
            cbuf[step].astype(jnp.float32) + ybuf[step].astype(jnp.float32)
        ).astype(jnp.bfloat16)
        obuf[step] = total
        for way in range(2):
            to_out(step, way, mine).start()
            out_ref[mine, out_cols(step, way)] = total[:, way * LANES:(way + 1) * LANES]

    project(0, d_ref[...])
    arrive(3, 2)
    project(1, dbuf[0])
    pair(0)

    @pl.loop(2, n)
    def _(step):
        @pl.when(step > 2)
        def _():
            arrive(2, step)

        pair(step - 1)

        @pl.when(step > 2)
        def _():
            settle(step - 3)
            arrive(3, step)

        project(step, dbuf[step - 1])

    pair(n - 1)
    settle(n - 3)
    settle(n - 2)
    settle(n - 1)

    @pl.loop(0, n - 1)
    def _(step):
        for stream in range(4):
            for way in range(2):
                hop(stream, way, step, True).wait_send()

    @pl.loop(0, n)
    def _(step):
        to_partner(step).wait_send()
        to_across(step).wait_send()
        for way in range(2):
            to_out(step, way, mine).wait_send()
            to_out(step, way, other).wait_recv()


def norm_kernel(b_ref, t_ref, gain_ref, bias_ref, out_ref):
    mixed = RESIDUAL_SCALE * t_ref[...].astype(jnp.float32) + b_ref[...].astype(jnp.float32)
    centered = mixed - jnp.mean(mixed, -1, keepdims=True)
    variance = jnp.mean(centered * centered, -1, keepdims=True)
    normed = centered * lax.rsqrt(variance + EPSILON) * gain_ref[...] + bias_ref[...]
    out_ref[...] = normed.astype(jnp.bfloat16)


def kernel_form(
    n, tokens, gate_weight, value_weight, gate_taps, value_taps, down_weight, norm_gain, norm_bias
):
    rows, width = tokens.shape
    depth, units = gate_weight.shape
    bf16, f32 = jnp.bfloat16, jnp.float32
    dma = pltpu.SemaphoreType.DMA
    branch = pl.pallas_call(
        functools.partial(branch_kernel, n),
        out_shape=jax.ShapeDtypeStruct((rows, width), bf16),
        in_specs=[pl.BlockSpec(memory_space=pl.ANY)]
        + [pl.BlockSpec(memory_space=pltpu.VMEM)] * 5,
        out_specs=pl.BlockSpec(memory_space=pltpu.VMEM),
        scratch_shapes=[
            pltpu.VMEM((rows, width), bf16),
            pltpu.VMEM((n - 1, depth, units), bf16),
            pltpu.VMEM((n - 1, depth, units), bf16),
            pltpu.VMEM((n - 1, units, depth), bf16),
            pltpu.VMEM((rows, units), f32),
            pltpu.VMEM((rows, units), f32),
            pltpu.VMEM((rows, units), bf16),
            pltpu.VMEM((n, rows, depth), bf16),
            pltpu.VMEM((n, rows // 2, depth), bf16),
            pltpu.VMEM((n, rows // 2, depth), bf16),
            pltpu.VMEM((n, rows // 2, depth), bf16),
            pltpu.VMEM((n, rows // 2, depth), bf16),
            dma((8, n - 1)),
            dma((8, n - 1)),
            dma((n,)),
            dma((n,)),
            dma((n,)),
            dma((n,)),
            dma((2, n)),
            dma((2, n)),
            dma,
        ],
        compiler_params=pltpu.CompilerParams(
            collective_id=0, has_side_effects=True, vmem_limit_bytes=VMEM_BYTES
        ),
        name="branch",
    )(tokens, gate_weight, value_weight, gate_taps, value_taps, down_weight)
    block = 256
    by_rows = pl.BlockSpec((block, width), lambda i: (i, 0))
    whole = pl.BlockSpec((1, width), lambda i: (0, 0))
    return pl.pallas_call(
        norm_kernel,
        grid=(rows // block,),
        out_shape=jax.ShapeDtypeStruct((rows, width), bf16),
        in_specs=[by_rows, by_rows, whole, whole],
        out_specs=by_rows,
        name="norm",
    )(branch, tokens, norm_gain.reshape(1, width), norm_bias.reshape(1, width))


def solution(mesh):
    n_fs, n_tp = mesh.shape["fs"], mesh.shape["tp"]

    def on_device(tokens, gate_weight, *rest):
        rows = tokens.shape[0]
        depth, units = gate_weight.shape
        fits = n_tp == 4 and n_fs % 2 == 0 and n_fs >= 6
        fits = fits and depth == 2 * LANES and units % LANES == 0 and rows % 512 == 0
        if fits:
            return kernel_form(n_fs, tokens, gate_weight, *rest)
        return collective_form(tokens, gate_weight, *rest)

    return jax.shard_map(
        on_device,
        mesh=mesh,
        in_specs=(
            P("fs", None),
            P("fs", "tp"),
            P("fs", "tp"),
            P(None, "tp"),
            P(None, "tp"),
            P("tp", "fs"),
            P(None),
            P(None),
        ),
        out_specs=P("fs", None),
        check_vma=False,
    )
```

```python
import functools

import jax
import jax.numpy as jnp
from jax import lax
from jax.experimental import pallas as pl
from jax.experimental.pallas import tpu as pltpu
from jax.sharding import PartitionSpec as P

EPSILON = 1e-05
RESIDUAL_SCALE = 8.0**0.25
LANES = 128
VMEM_BYTES = 67043328


def rounded(values):
    return lax.optimization_barrier(values.astype(jnp.bfloat16)).astype(jnp.float32)


def centred_conv(values, taps):
    padded = jnp.pad(values, ((1, 1), (0, 0)))
    return padded[:-2] * taps[0] + padded[1:-1] * taps[1] + padded[2:] * taps[2]


def finish(summed, residual, norm_gain, norm_bias):
    mixed = RESIDUAL_SCALE * residual.astype(jnp.float32) + rounded(summed)
    centered = mixed - jnp.mean(mixed, -1, keepdims=True)
    variance = jnp.mean(centered * centered, -1, keepdims=True)
    normed = centered * lax.rsqrt(variance + EPSILON) * norm_gain + norm_bias
    return normed.astype(jnp.bfloat16)


def collective_form(
    tokens, gate_weight, value_weight, gate_taps, value_taps, down_weight, norm_gain, norm_bias
):
    def add_rows(portion):
        return jnp.dot(tokens, portion, preferred_element_type=jnp.float32)

    gate_sum = add_rows(lax.all_gather(gate_weight, "fs", axis=0, tiled=True))
    value_sum = add_rows(lax.all_gather(value_weight, "fs", axis=0, tiled=True))
    gate_conv = centred_conv(rounded(gate_sum), gate_taps.astype(jnp.float32))
    value_conv = centred_conv(rounded(value_sum), value_taps.astype(jnp.float32))
    hidden = (jax.nn.silu(gate_conv) * value_conv).astype(jnp.bfloat16)
    partials = rounded(
        jnp.dot(
            hidden,
            lax.all_gather(down_weight, "fs", axis=1, tiled=True),
            preferred_element_type=jnp.float32,
        )
    )
    shares = lax.psum_scatter(
        partials.astype(jnp.bfloat16), "tp", scatter_dimension=0, tiled=True
    ).astype(jnp.float32)
    share_rows = shares.shape[0]
    own_rows = lax.dynamic_slice_in_dim(tokens, lax.axis_index("tp") * share_rows, share_rows, 0)
    normed_share = finish(shares, own_rows, norm_gain, norm_bias)
    return lax.all_gather(normed_share, "tp", axis=0, tiled=True)


def branch_kernel(
    n, t_hbm, g_ref, v_ref, gt_ref, vt_ref, d_ref, out_ref,
    t_ref, gbuf, vbuf, dbuf, acc_g, acc_v, hid, pbuf, rbuf, cbuf, ybuf, obuf,
    w_send, w_recv, c_send, c_recv, y_send, y_recv, o_send, o_recv, l_sem, t_sem,
):
    rows, units = hid.shape
    half_rows = rows // 2
    tile = 256
    fs = lax.axis_index("fs")
    tp = lax.axis_index("tp")
    core = lax.rem(tp, 2)
    partner = tp + 1 - 2 * core
    across = lax.rem(tp + 2, 4)
    half_n = n // 2

    x, z = lax.rem(fs, 2), lax.div(fs, 2)
    pos = (1 - x) * z + x * (n - 1 - z)

    def at_pos(p):
        p = lax.rem(p, n)
        down = lax.div(p, half_n)
        return (1 - down) * 2 * p + down * (2 * (n - 1 - p) + 1)

    right, left = at_pos(pos + 1), at_pos(pos + n - 1)

    barrier = pltpu.get_barrier_semaphore()
    for target in ({"fs": left}, {"fs": right}, {"tp": partner}, {"tp": across}):
        pl.semaphore_signal(
            barrier, inc=1, device_id=target, device_id_type=pl.DeviceIdType.MESH
        )
    pl.semaphore_wait(barrier, 4)

    streams = ((g_ref, gbuf), (v_ref, vbuf), (d_ref, dbuf), (d_ref, dbuf))
    half_units = units // 2

    def hop(stream, way, step, first=False):
        own, slots = streams[stream]
        part = pl.ds(way * LANES, LANES)
        where = (part, slice(None))
        if stream >= 2:
            where = (pl.ds((stream - 2) * half_units, half_units), part)
        source = own.at[where] if first else slots.at[(step - 1,) + where]
        k = stream * 2 + way
        return pltpu.make_async_remote_copy(
            src_ref=source,
            dst_ref=slots.at[(step,) + where],
            send_sem=w_send.at[k, step],
            recv_sem=w_recv.at[k, step],
            device_id={"fs": right if way == 0 else left},
            device_id_type=pl.DeviceIdType.MESH,
        )

    def begin(stream):
        for way in range(2):
            hop(stream, way, 0, True).start()

    def arrive(stream, step):
        for way in range(2):
            hop(stream, way, step - 1, True).wait_recv()

            @pl.when(step < n - 1)
            def _():
                hop(stream, way, step).start()

    begin(0)
    begin(1)
    load = pltpu.make_async_copy(t_hbm, t_ref, t_sem)
    load.start()
    load.wait()

    def token_tile(r, step):
        row = pl.ds(pl.multiple_of(r * tile, tile), tile)
        a = pl.multiple_of(at_pos(pos + n - step) * 2 * LANES, LANES)
        b = pl.multiple_of(at_pos(pos + step) * 2 * LANES + LANES, LANES)
        return row, jnp.concatenate(
            [t_ref[row, pl.ds(a, LANES)], t_ref[row, pl.ds(b, LANES)]], axis=1
        )

    @pl.loop(0, rows // tile)
    def _(r):
        row, lhs = token_tile(r, 0)
        acc_g[row, :] = jnp.dot(lhs, g_ref[...], preferred_element_type=jnp.float32)
        acc_v[row, :] = jnp.dot(lhs, v_ref[...], preferred_element_type=jnp.float32)

    @pl.loop(1, n)
    def _(step):
        arrive(0, step)
        arrive(1, step)

        @pl.when(step == n - 2)
        def _():
            begin(2)
            begin(3)

        @pl.loop(0, rows // tile)
        def _(r):
            row, lhs = token_tile(r, step)
            acc_g[row, :] += jnp.dot(lhs, gbuf[step - 1], preferred_element_type=jnp.float32)
            acc_v[row, :] += jnp.dot(lhs, vbuf[step - 1], preferred_element_type=jnp.float32)

    row_id = lax.broadcasted_iota(jnp.int32, (rows, LANES), 0)

    def conv(acc, taps, cols):
        v = acc[:, cols].astype(jnp.bfloat16).astype(jnp.float32)
        c = taps[:, cols].astype(jnp.float32)
        before = jnp.where(row_id == 0, 0.0, pltpu.roll(v, 1, 0))
        after = jnp.where(row_id == rows - 1, 0.0, pltpu.roll(v, rows - 1, 0))
        return before * c[0:1] + v * c[1:2] + after * c[2:3]

    chunks = units // LANES

    @pl.loop(0, chunks)
    def _(i):
        cols = pl.ds(pl.multiple_of(i * LANES, LANES), LANES)
        gate = conv(acc_g, gt_ref, cols)
        value = conv(acc_v, vt_ref, cols)
        hid[:, cols] = (gate / (1.0 + jnp.exp(-gate)) * value).astype(jnp.bfloat16)

        @pl.when(i == chunks // 4)
        def _():
            arrive(2, 1)

        @pl.when(i == chunks // 2)
        def _():
            arrive(3, 1)

        @pl.when(i == chunks - 2)
        def _():
            arrive(2, 2)

    mine = pl.ds(pl.multiple_of(core * half_rows, half_rows), half_rows)
    other = pl.ds(pl.multiple_of((1 - core) * half_rows, half_rows), half_rows)

    def to_partner(step):
        return pltpu.make_async_remote_copy(
            src_ref=pbuf.at[step, other],
            dst_ref=rbuf.at[step],
            send_sem=c_send.at[step],
            recv_sem=c_recv.at[step],
            device_id={"tp": partner},
            device_id_type=pl.DeviceIdType.MESH,
        )

    def to_across(step):
        return pltpu.make_async_remote_copy(
            src_ref=cbuf.at[step],
            dst_ref=ybuf.at[step],
            send_sem=y_send.at[step],
            recv_sem=y_recv.at[step],
            device_id={"tp": across},
            device_id_type=pl.DeviceIdType.MESH,
        )

    def out_cols(step, way):
        owner = at_pos(pos + n - step) if way == 0 else at_pos(pos + step)
        return pl.ds(pl.multiple_of(owner * 2 * LANES + way * LANES, LANES), LANES)

    def to_out(step, way, where):
        cols = out_cols(step, way)
        return pltpu.make_async_remote_copy(
            src_ref=obuf.at[step, :, pl.ds(way * LANES, LANES)],
            dst_ref=out_ref.at[where, cols],
            send_sem=o_send.at[way, step],
            recv_sem=o_recv.at[way, step],
            device_id={"tp": partner},
            device_id_type=pl.DeviceIdType.MESH,
        )

    def to_own(step, way):
        return pltpu.make_async_copy(
            obuf.at[step, :, pl.ds(way * LANES, LANES)],
            out_ref.at[mine, out_cols(step, way)],
            l_sem.at[way, step],
        )

    def project(step, weight):
        def rows_from(first):
            @pl.loop(0, half_rows // tile)
            def _(r):
                row = pl.ds(pl.multiple_of(first * half_rows + r * tile, tile), tile)
                pbuf[step, row, :] = jnp.dot(
                    hid[row, :], weight, preferred_element_type=jnp.float32
                ).astype(jnp.bfloat16)

        rows_from(1 - core)
        to_partner(step).start()
        rows_from(core)

    def pair(step):
        to_partner(step).wait_recv()
        cbuf[step] = (
            pbuf[step, mine].astype(jnp.float32) + rbuf[step].astype(jnp.float32)
        ).astype(jnp.bfloat16)
        to_across(step).start()

    def settle(step):
        to_across(step).wait_recv()
        obuf[step] = (
            cbuf[step].astype(jnp.float32) + ybuf[step].astype(jnp.float32)
        ).astype(jnp.bfloat16)
        for way in range(2):
            to_out(step, way, mine).start()
            to_own(step, way).start()

    project(0, d_ref[...])
    arrive(3, 2)
    project(1, dbuf[0])
    pair(0)

    @pl.loop(2, n)
    def _(step):
        @pl.when(step > 2)
        def _():
            arrive(2, step)

        pair(step - 1)

        @pl.when(step > 2)
        def _():
            settle(step - 3)
            arrive(3, step)

        project(step, dbuf[step - 1])

    pair(n - 1)
    settle(n - 3)
    settle(n - 2)
    settle(n - 1)

    @pl.loop(0, n - 1)
    def _(step):
        for stream in range(4):
            for way in range(2):
                hop(stream, way, step, True).wait_send()

    @pl.loop(0, n)
    def _(step):
        to_partner(step).wait_send()
        to_across(step).wait_send()
        for way in range(2):
            to_out(step, way, mine).wait_send()
            to_own(step, way).wait()
            to_out(step, way, other).wait_recv()


NORM_ROWS = 128


def norm_kernel(b_hbm, t_hbm, gain_ref, bias_ref, out_hbm, b_ref, t_ref, o_ref, in_sem, out_sem):
    count = b_ref.shape[0] // NORM_ROWS

    def chunk(i):
        return pl.ds(pl.multiple_of(i * NORM_ROWS, NORM_ROWS), NORM_ROWS)

    def loads(i):
        part = chunk(i)
        return (
            pltpu.make_async_copy(b_hbm.at[part], b_ref.at[part], in_sem.at[0, i]),
            pltpu.make_async_copy(t_hbm.at[part], t_ref.at[part], in_sem.at[1, i]),
        )

    def store(i):
        part = chunk(i)
        return pltpu.make_async_copy(o_ref.at[part], out_hbm.at[part], out_sem.at[i])

    for i in range(count):
        for load in loads(i):
            load.start()

    @pl.loop(0, count)
    def _(i):
        for load in loads(i):
            load.wait()
        part = chunk(i)
        mixed = RESIDUAL_SCALE * t_ref[part, :].astype(jnp.float32)
        mixed += b_ref[part, :].astype(jnp.float32)
        centered = mixed - jnp.mean(mixed, -1, keepdims=True)
        variance = jnp.mean(centered * centered, -1, keepdims=True)
        normed = centered * lax.rsqrt(variance + EPSILON) * gain_ref[...] + bias_ref[...]
        o_ref[part, :] = normed.astype(jnp.bfloat16)
        store(i).start()

    @pl.loop(0, count)
    def _(i):
        store(i).wait()


def kernel_form(
    n, tokens, gate_weight, value_weight, gate_taps, value_taps, down_weight, norm_gain, norm_bias
):
    rows, width = tokens.shape
    depth, units = gate_weight.shape
    bf16, f32 = jnp.bfloat16, jnp.float32
    dma = pltpu.SemaphoreType.DMA
    branch = pl.pallas_call(
        functools.partial(branch_kernel, n),
        out_shape=jax.ShapeDtypeStruct((rows, width), bf16),
        in_specs=[pl.BlockSpec(memory_space=pl.ANY)]
        + [pl.BlockSpec(memory_space=pltpu.VMEM)] * 5,
        out_specs=pl.BlockSpec(memory_space=pl.ANY),
        scratch_shapes=[
            pltpu.VMEM((rows, width), bf16),
            pltpu.VMEM((n - 1, depth, units), bf16),
            pltpu.VMEM((n - 1, depth, units), bf16),
            pltpu.VMEM((n - 1, units, depth), bf16),
            pltpu.VMEM((rows, units), f32),
            pltpu.VMEM((rows, units), f32),
            pltpu.VMEM((rows, units), bf16),
            pltpu.VMEM((n, rows, depth), bf16),
            pltpu.VMEM((n, rows // 2, depth), bf16),
            pltpu.VMEM((n, rows // 2, depth), bf16),
            pltpu.VMEM((n, rows // 2, depth), bf16),
            pltpu.VMEM((n, rows // 2, depth), bf16),
            dma((8, n - 1)),
            dma((8, n - 1)),
            dma((n,)),
            dma((n,)),
            dma((n,)),
            dma((n,)),
            dma((2, n)),
            dma((2, n)),
            dma((2, n)),
            dma,
        ],
        compiler_params=pltpu.CompilerParams(
            collective_id=0, has_side_effects=True, vmem_limit_bytes=VMEM_BYTES
        ),
        name="branch",
    )(tokens, gate_weight, value_weight, gate_taps, value_taps, down_weight)
    anywhere = pl.BlockSpec(memory_space=pl.ANY)
    vector = pl.BlockSpec(memory_space=pltpu.VMEM)
    count = rows // NORM_ROWS
    return pl.pallas_call(
        norm_kernel,
        out_shape=jax.ShapeDtypeStruct((rows, width), bf16),
        in_specs=[anywhere, anywhere, vector, vector],
        out_specs=anywhere,
        scratch_shapes=[pltpu.VMEM((rows, width), bf16)] * 3 + [dma((2, count)), dma((count,))],
        compiler_params=pltpu.CompilerParams(vmem_limit_bytes=VMEM_BYTES),
        name="norm",
    )(branch, tokens, norm_gain.reshape(1, width), norm_bias.reshape(1, width))


def solution(mesh):
    n_fs, n_tp = mesh.shape["fs"], mesh.shape["tp"]

    def on_device(tokens, gate_weight, *rest):
        rows = tokens.shape[0]
        depth, units = gate_weight.shape
        fits = n_tp == 4 and n_fs % 2 == 0 and n_fs >= 6
        fits = fits and depth == 2 * LANES and units % LANES == 0 and rows % 512 == 0
        if fits:
            return kernel_form(n_fs, tokens, gate_weight, *rest)
        return collective_form(tokens, gate_weight, *rest)

    return jax.shard_map(
        on_device,
        mesh=mesh,
        in_specs=(
            P("fs", None),
            P("fs", "tp"),
            P("fs", "tp"),
            P(None, "tp"),
            P(None, "tp"),
            P("tp", "fs"),
            P(None),
            P(None),
        ),
        out_specs=P("fs", None),
        check_vma=False,
    )
```

```python
import functools

import jax
import jax.numpy as jnp
from jax import lax
from jax.experimental import pallas as pl
from jax.experimental.pallas import tpu as pltpu
from jax.sharding import PartitionSpec as P

EPSILON = 1e-05
RESIDUAL_SCALE = 8.0**0.25
LANES = 128
VMEM_BYTES = 67043328


def rounded(values):
    return lax.optimization_barrier(values.astype(jnp.bfloat16)).astype(jnp.float32)


def centred_conv(values, taps):
    padded = jnp.pad(values, ((1, 1), (0, 0)))
    return padded[:-2] * taps[0] + padded[1:-1] * taps[1] + padded[2:] * taps[2]


def finish(summed, residual, norm_gain, norm_bias):
    mixed = RESIDUAL_SCALE * residual.astype(jnp.float32) + rounded(summed)
    centered = mixed - jnp.mean(mixed, -1, keepdims=True)
    variance = jnp.mean(centered * centered, -1, keepdims=True)
    normed = centered * lax.rsqrt(variance + EPSILON) * norm_gain + norm_bias
    return normed.astype(jnp.bfloat16)


def collective_form(
    tokens, gate_weight, value_weight, gate_taps, value_taps, down_weight, norm_gain, norm_bias
):
    def add_rows(portion):
        return jnp.dot(tokens, portion, preferred_element_type=jnp.float32)

    gate_sum = add_rows(lax.all_gather(gate_weight, "fs", axis=0, tiled=True))
    value_sum = add_rows(lax.all_gather(value_weight, "fs", axis=0, tiled=True))
    gate_conv = centred_conv(rounded(gate_sum), gate_taps.astype(jnp.float32))
    value_conv = centred_conv(rounded(value_sum), value_taps.astype(jnp.float32))
    hidden = (jax.nn.silu(gate_conv) * value_conv).astype(jnp.bfloat16)
    partials = rounded(
        jnp.dot(
            hidden,
            lax.all_gather(down_weight, "fs", axis=1, tiled=True),
            preferred_element_type=jnp.float32,
        )
    )
    shares = lax.psum_scatter(
        partials.astype(jnp.bfloat16), "tp", scatter_dimension=0, tiled=True
    ).astype(jnp.float32)
    share_rows = shares.shape[0]
    own_rows = lax.dynamic_slice_in_dim(tokens, lax.axis_index("tp") * share_rows, share_rows, 0)
    normed_share = finish(shares, own_rows, norm_gain, norm_bias)
    return lax.all_gather(normed_share, "tp", axis=0, tiled=True)


def branch_kernel(
    n, t_hbm, g_hbm, v_hbm, gt_ref, vt_ref, d_hbm, out_ref,
    t_ref, g_ref, v_ref, d_ref, gbuf, vbuf, dbuf, acc_g, acc_v, hid, pbuf, rbuf, cbuf, ybuf, obuf,
    w_send, w_recv, c_send, c_recv, y_send, y_recv, o_send, o_recv, l_sem, t_sem,
):
    rows, units = hid.shape
    half_rows = rows // 2
    tile = 256
    fs = lax.axis_index("fs")
    tp = lax.axis_index("tp")
    core = lax.rem(tp, 2)
    partner = tp + 1 - 2 * core
    across = lax.rem(tp + 2, 4)
    half_n = n // 2

    x, z = lax.rem(fs, 2), lax.div(fs, 2)
    pos = (1 - x) * z + x * (n - 1 - z)

    def at_pos(p):
        p = lax.rem(p, n)
        down = lax.div(p, half_n)
        return (1 - down) * 2 * p + down * (2 * (n - 1 - p) + 1)

    right, left = at_pos(pos + 1), at_pos(pos + n - 1)

    pairs = ((g_hbm, g_ref), (v_hbm, v_ref), (t_hbm, t_ref), (d_hbm, d_ref))
    loads = [pltpu.make_async_copy(a, b, t_sem.at[i]) for i, (a, b) in enumerate(pairs)]
    for load in loads:
        load.start()

    barrier = pltpu.get_barrier_semaphore()
    for target in ({"fs": left}, {"fs": right}, {"tp": partner}, {"tp": across}):
        pl.semaphore_signal(
            barrier, inc=1, device_id=target, device_id_type=pl.DeviceIdType.MESH
        )
    pl.semaphore_wait(barrier, 4)

    streams = ((g_ref, gbuf), (v_ref, vbuf), (d_ref, dbuf), (d_ref, dbuf))
    half_units = units // 2

    def hop(stream, way, step, first=False):
        own, slots = streams[stream]
        part = pl.ds(way * LANES, LANES)
        where = (part, slice(None))
        if stream >= 2:
            where = (pl.ds((stream - 2) * half_units, half_units), part)
        source = own.at[where] if first else slots.at[(step - 1,) + where]
        k = stream * 2 + way
        return pltpu.make_async_remote_copy(
            src_ref=source,
            dst_ref=slots.at[(step,) + where],
            send_sem=w_send.at[k, step],
            recv_sem=w_recv.at[k, step],
            device_id={"fs": right if way == 0 else left},
            device_id_type=pl.DeviceIdType.MESH,
        )

    def begin(stream):
        for way in range(2):
            hop(stream, way, 0, True).start()

    def arrive(stream, step):
        for way in range(2):
            hop(stream, way, step - 1, True).wait_recv()

            @pl.when(step < n - 1)
            def _():
                hop(stream, way, step).start()

    loads[0].wait()
    begin(0)
    loads[1].wait()
    begin(1)
    loads[2].wait()
    loads[3].wait()

    def token_tile(r, step):
        row = pl.ds(pl.multiple_of(r * tile, tile), tile)
        a = pl.multiple_of(at_pos(pos + n - step) * 2 * LANES, LANES)
        b = pl.multiple_of(at_pos(pos + step) * 2 * LANES + LANES, LANES)
        return row, jnp.concatenate(
            [t_ref[row, pl.ds(a, LANES)], t_ref[row, pl.ds(b, LANES)]], axis=1
        )

    @pl.loop(0, rows // tile)
    def _(r):
        row, lhs = token_tile(r, 0)
        acc_g[row, :] = jnp.dot(lhs, g_ref[...], preferred_element_type=jnp.float32)
        acc_v[row, :] = jnp.dot(lhs, v_ref[...], preferred_element_type=jnp.float32)

    @pl.loop(1, n)
    def _(step):
        arrive(0, step)
        arrive(1, step)

        @pl.when(step == n - 2)
        def _():
            begin(2)
            begin(3)

        @pl.loop(0, rows // tile)
        def _(r):
            row, lhs = token_tile(r, step)
            acc_g[row, :] += jnp.dot(lhs, gbuf[step - 1], preferred_element_type=jnp.float32)
            acc_v[row, :] += jnp.dot(lhs, vbuf[step - 1], preferred_element_type=jnp.float32)

    row_id = lax.broadcasted_iota(jnp.int32, (rows, LANES), 0)

    def conv(acc, taps, cols):
        v = acc[:, cols].astype(jnp.bfloat16).astype(jnp.float32)
        c = taps[:, cols].astype(jnp.float32)
        before = jnp.where(row_id == 0, 0.0, pltpu.roll(v, 1, 0))
        after = jnp.where(row_id == rows - 1, 0.0, pltpu.roll(v, rows - 1, 0))
        return before * c[0:1] + v * c[1:2] + after * c[2:3]

    chunks = units // LANES

    @pl.loop(0, chunks)
    def _(i):
        cols = pl.ds(pl.multiple_of(i * LANES, LANES), LANES)
        gate = conv(acc_g, gt_ref, cols)
        value = conv(acc_v, vt_ref, cols)
        hid[:, cols] = (gate / (1.0 + jnp.exp(-gate)) * value).astype(jnp.bfloat16)

        @pl.when(i == chunks // 4)
        def _():
            arrive(2, 1)

        @pl.when(i == chunks // 2)
        def _():
            arrive(3, 1)

        @pl.when(i == chunks - 2)
        def _():
            arrive(2, 2)

    mine = pl.ds(pl.multiple_of(core * half_rows, half_rows), half_rows)
    other = pl.ds(pl.multiple_of((1 - core) * half_rows, half_rows), half_rows)

    def to_partner(step):
        return pltpu.make_async_remote_copy(
            src_ref=pbuf.at[step, other],
            dst_ref=rbuf.at[step],
            send_sem=c_send.at[step],
            recv_sem=c_recv.at[step],
            device_id={"tp": partner},
            device_id_type=pl.DeviceIdType.MESH,
        )

    def to_across(step):
        return pltpu.make_async_remote_copy(
            src_ref=cbuf.at[step],
            dst_ref=ybuf.at[step],
            send_sem=y_send.at[step],
            recv_sem=y_recv.at[step],
            device_id={"tp": across},
            device_id_type=pl.DeviceIdType.MESH,
        )

    def out_cols(step, way):
        owner = at_pos(pos + n - step) if way == 0 else at_pos(pos + step)
        return pl.ds(pl.multiple_of(owner * 2 * LANES + way * LANES, LANES), LANES)

    def to_out(step, way, where):
        cols = out_cols(step, way)
        return pltpu.make_async_remote_copy(
            src_ref=obuf.at[step, :, pl.ds(way * LANES, LANES)],
            dst_ref=out_ref.at[where, cols],
            send_sem=o_send.at[way, step],
            recv_sem=o_recv.at[way, step],
            device_id={"tp": partner},
            device_id_type=pl.DeviceIdType.MESH,
        )

    def to_own(step, way):
        return pltpu.make_async_copy(
            obuf.at[step, :, pl.ds(way * LANES, LANES)],
            out_ref.at[mine, out_cols(step, way)],
            l_sem.at[way, step],
        )

    def project(step, weight):
        def rows_from(first):
            @pl.loop(0, half_rows // tile)
            def _(r):
                row = pl.ds(pl.multiple_of(first * half_rows + r * tile, tile), tile)
                pbuf[step, row, :] = jnp.dot(
                    hid[row, :], weight, preferred_element_type=jnp.float32
                ).astype(jnp.bfloat16)

        rows_from(1 - core)
        to_partner(step).start()
        rows_from(core)

    def pair(step):
        to_partner(step).wait_recv()
        cbuf[step] = (
            pbuf[step, mine].astype(jnp.float32) + rbuf[step].astype(jnp.float32)
        ).astype(jnp.bfloat16)
        to_across(step).start()

    def settle(step):
        to_across(step).wait_recv()
        obuf[step] = (
            cbuf[step].astype(jnp.float32) + ybuf[step].astype(jnp.float32)
        ).astype(jnp.bfloat16)
        for way in range(2):
            to_out(step, way, mine).start()
            to_own(step, way).start()

    project(0, d_ref[...])
    arrive(3, 2)
    project(1, dbuf[0])
    pair(0)

    @pl.loop(2, n)
    def _(step):
        @pl.when(step > 2)
        def _():
            arrive(2, step)

        pair(step - 1)

        @pl.when(step > 2)
        def _():
            settle(step - 3)
            arrive(3, step)

        project(step, dbuf[step - 1])

    pair(n - 1)
    settle(n - 3)
    settle(n - 2)
    settle(n - 1)

    @pl.loop(0, n - 1)
    def _(step):
        for stream in range(4):
            for way in range(2):
                hop(stream, way, step, True).wait_send()

    @pl.loop(0, n)
    def _(step):
        to_partner(step).wait_send()
        to_across(step).wait_send()
        for way in range(2):
            to_out(step, way, mine).wait_send()
            to_own(step, way).wait()
            to_out(step, way, other).wait_recv()


NORM_ROWS = 128


def norm_kernel(b_hbm, t_hbm, gain_ref, bias_ref, out_hbm, b_ref, t_ref, o_ref, in_sem, out_sem):
    count = b_ref.shape[0] // NORM_ROWS

    def chunk(i):
        return pl.ds(pl.multiple_of(i * NORM_ROWS, NORM_ROWS), NORM_ROWS)

    def loads(i):
        part = chunk(i)
        return (
            pltpu.make_async_copy(b_hbm.at[part], b_ref.at[part], in_sem.at[0, i]),
            pltpu.make_async_copy(t_hbm.at[part], t_ref.at[part], in_sem.at[1, i]),
        )

    def store(i):
        part = chunk(i)
        return pltpu.make_async_copy(o_ref.at[part], out_hbm.at[part], out_sem.at[i])

    for i in range(count):
        for load in loads(i):
            load.start()

    @pl.loop(0, count)
    def _(i):
        for load in loads(i):
            load.wait()
        part = chunk(i)
        mixed = RESIDUAL_SCALE * t_ref[part, :].astype(jnp.float32)
        mixed += b_ref[part, :].astype(jnp.float32)
        centered = mixed - jnp.mean(mixed, -1, keepdims=True)
        variance = jnp.mean(centered * centered, -1, keepdims=True)
        normed = centered * lax.rsqrt(variance + EPSILON) * gain_ref[...] + bias_ref[...]
        o_ref[part, :] = normed.astype(jnp.bfloat16)
        store(i).start()

    @pl.loop(0, count)
    def _(i):
        store(i).wait()


def kernel_form(
    n, tokens, gate_weight, value_weight, gate_taps, value_taps, down_weight, norm_gain, norm_bias
):
    rows, width = tokens.shape
    depth, units = gate_weight.shape
    bf16, f32 = jnp.bfloat16, jnp.float32
    dma = pltpu.SemaphoreType.DMA
    anywhere = pl.BlockSpec(memory_space=pl.ANY)
    vector = pl.BlockSpec(memory_space=pltpu.VMEM)
    branch = pl.pallas_call(
        functools.partial(branch_kernel, n),
        out_shape=jax.ShapeDtypeStruct((rows, width), bf16),
        in_specs=[anywhere] * 3 + [vector] * 2 + [anywhere],
        out_specs=pl.BlockSpec(memory_space=pl.ANY),
        scratch_shapes=[
            pltpu.VMEM((rows, width), bf16),
            pltpu.VMEM((depth, units), bf16),
            pltpu.VMEM((depth, units), bf16),
            pltpu.VMEM((units, depth), bf16),
            pltpu.VMEM((n - 1, depth, units), bf16),
            pltpu.VMEM((n - 1, depth, units), bf16),
            pltpu.VMEM((n - 1, units, depth), bf16),
            pltpu.VMEM((rows, units), f32),
            pltpu.VMEM((rows, units), f32),
            pltpu.VMEM((rows, units), bf16),
            pltpu.VMEM((n, rows, depth), bf16),
            pltpu.VMEM((n, rows // 2, depth), bf16),
            pltpu.VMEM((n, rows // 2, depth), bf16),
            pltpu.VMEM((n, rows // 2, depth), bf16),
            pltpu.VMEM((n, rows // 2, depth), bf16),
            dma((8, n - 1)),
            dma((8, n - 1)),
            dma((n,)),
            dma((n,)),
            dma((n,)),
            dma((n,)),
            dma((2, n)),
            dma((2, n)),
            dma((2, n)),
            dma((4,)),
        ],
        compiler_params=pltpu.CompilerParams(
            collective_id=0, has_side_effects=True, vmem_limit_bytes=VMEM_BYTES
        ),
        name="branch",
    )(tokens, gate_weight, value_weight, gate_taps, value_taps, down_weight)
    count = rows // NORM_ROWS
    return pl.pallas_call(
        norm_kernel,
        out_shape=jax.ShapeDtypeStruct((rows, width), bf16),
        in_specs=[anywhere, anywhere, vector, vector],
        out_specs=anywhere,
        scratch_shapes=[pltpu.VMEM((rows, width), bf16)] * 3 + [dma((2, count)), dma((count,))],
        compiler_params=pltpu.CompilerParams(vmem_limit_bytes=VMEM_BYTES),
        name="norm",
    )(branch, tokens, norm_gain.reshape(1, width), norm_bias.reshape(1, width))


def solution(mesh):
    n_fs, n_tp = mesh.shape["fs"], mesh.shape["tp"]

    def on_device(tokens, gate_weight, *rest):
        rows = tokens.shape[0]
        depth, units = gate_weight.shape
        fits = n_tp == 4 and n_fs % 2 == 0 and n_fs >= 6
        fits = fits and depth == 2 * LANES and units % LANES == 0 and rows % 512 == 0
        if fits:
            return kernel_form(n_fs, tokens, gate_weight, *rest)
        return collective_form(tokens, gate_weight, *rest)

    return jax.shard_map(
        on_device,
        mesh=mesh,
        in_specs=(
            P("fs", None),
            P("fs", "tp"),
            P("fs", "tp"),
            P(None, "tp"),
            P(None, "tp"),
            P("tp", "fs"),
            P(None),
            P(None),
        ),
        out_specs=P("fs", None),
        check_vma=False,
    )
```
